32 devices in a mesh: grp: 2 (over x), ep: 16 (over z, y, core).
Axes of the slice: x: 2, y: 2, z: 4, core: 2. Of those that a mesh axis runs over, the one named last changes fastest.
Arguments:
- tokens: bfloat16 [32, 2048], P(('grp', 'ep')), parts along dimension 0, may hold values from -6 to 6
- cache_latent: bfloat16 [32, 3072, 512], P(('grp', 'ep')), parts along dimension 0, may hold values from -6 to 6
- cache_rope: bfloat16 [32, 32, 3072], P(('grp', 'ep')), parts along dimension 0, may hold values from -1000 to 1000
- lengths: int32 [32], P(('grp', 'ep')), parts along dimension 0, may hold values from 384 to 3072, as said below
- w_query: bfloat16 [2048, 1536], P('ep'), may hold values from -0.125 to 0.125
- w_latent: bfloat16 [2048, 512], P('ep'), may hold values from -0.125 to 0.125
- w_rope: bfloat16 [2048, 32], P('ep'), may hold values from -0.125 to 0.125
- w_absorb: bfloat16 [512, 1024], replicated, may hold values from -0.25 to 0.25
- w_value: bfloat16 [512, 1024], replicated, may hold values from -0.25 to 0.25
- w_output: bfloat16 [1024, 2048], P('ep'), may hold values from -0.1875 to 0.1875
- gain_attn: float32 [2048], replicated, may hold values from 0.1 to 1.9
- gain_latent: float32 [512], replicated, may hold values from 0.1 to 1.9
- gain_moe: float32 [2048], replicated, may hold values from 0.1 to 1.9
- routes: int32 [32, 2], P(('grp', 'ep')), parts along dimension 0, may hold values from 0 to 15, all different within a row; in each aligned block of 16 rows (0 to 15, 16 to 31, ...) at most 4 rows name the same one
- route_scores: float32 [32, 2], P(('grp', 'ep')), parts along dimension 0, may hold values from 0.2 to 1
- w_gate: bfloat16 [16, 2048, 512], P('ep'), may hold values from -0.125 to 0.125
- w_up: bfloat16 [16, 2048, 512], P('ep'), may hold values from -0.125 to 0.125
- w_down: bfloat16 [16, 512, 2048], P('ep'), may hold values from -0.25 to 0.25
Outputs:
- mixed: bfloat16 [32, 2048], P(('grp', 'ep')), parts along dimension 0
- new_latent: bfloat16 [32, 512], P(('grp', 'ep')), parts along dimension 0
- new_rope: bfloat16 [32, 32], P(('grp', 'ep')), parts along dimension 0
The draws below stay inside these ranges and needn't reach their ends.
There are 2 independent parts, one for each index of `grp`. The reference program is written for one: setup_inputs(seed, part) draws one part's arguments, and reference() takes and returns one part's arrays. A program takes and returns all parts, laid end to end along the dimension named above; an argument that names none is the same for every part. Nothing has to cross between parts.
Inputs may be any that keep to these rules, and one draw needn't show every extreme that they name: `routes`: each row names 2 different experts; over one part's 16 tokens no expert is named by more than 4 rows, a bound that some block reaches. `lengths`: some sequence has all 3072 positions filled.
All inputs are finite; a program needn't handle non-finite values.
Results may differ from the reference program's by a relative error of at most 0.013.
Values may be sent and summed in bfloat16 or wider, within the bound.
A program may use at most 64 MiB of HBM per device.

```python
import math
import jax
import jax.numpy as jnp
import numpy as np
from jax import lax

D = 2048
HEADS = 16
NOPE = 64
ROPE = 32
VDIM = 64
LATENT = 512
FF = 512
TOPK = 2
CACHE = 3072
SEQS = 16
EXPERTS = 16
CAP = 4


def draw_cache_rope(key, part):
    k_base = jax.random.fold_in(jax.random.fold_in(key, 31), 0)
    base = jnp.clip(jax.random.normal(k_base, (SEQS, ROPE, CACHE), jnp.float32), -6.0, 6.0)
    return base.astype(jnp.bfloat16)


def draw_lengths(key, part):
    k_len, k_full = jax.random.split(jax.random.fold_in(key, 23))
    values = jax.random.randint(k_len, (SEQS,), CACHE // 8, CACHE + 1)
    chosen = jax.random.randint(k_full, (), 0, SEQS)
    values = jnp.where(jnp.arange(SEQS) == chosen, CACHE, values)
    return values.astype(jnp.int32)


def block_scale(own_key, extent, shards, low, top_value):
    def one(dim, shards_of):
        draws = jax.random.uniform(jax.random.fold_in(jax.random.fold_in(own_key, 6), dim), (shards_of,), jnp.float32, low / len(shards), top_value / len(shards))
        return jnp.repeat(jnp.exp(draws), extent[dim] // shards_of).reshape((-1,) + (1,) * (len(extent) - dim - 1))

    level = one(*shards[0])
    for cut in shards[1:]:
        level = level * one(*cut)
    return level


def assign_block(own_key, own, number, rows, number_of, top, most, lean):
    order = jax.random.permutation(own_key, number_of)
    crowded, ordinary = portions_of(number_of, rows * top, most, lean, True), portions_of(number_of, rows * top, most, lean, False)
    places = jnp.arange(number_of)

    def named(sizes, turn):
        used = int((sizes > 0).sum())
        fixed = max(1, used // 4)
        moved = fixed + (places - fixed + turn * (used - fixed)) % max(1, number_of - fixed)
        return jnp.zeros((number_of,), jnp.int32).at[order[jnp.where(places < fixed, places, moved)]].set(jnp.asarray(sizes, jnp.int32))

    sizes = jnp.where(number % 4 == 0, named(crowded, number // 4), named(ordinary, number - number // 4 - 1))
    mixed = jax.random.permutation(jax.random.fold_in(own, 3), number_of)
    donor, receiver = mixed[0:number_of // 2 * 2:2], mixed[1:number_of // 2 * 2:2]
    margin = jnp.minimum(sizes[donor] - 1, most - sizes[receiver]) // 2
    margin = jnp.where((donor == order[0]) | (receiver == order[0]) | (sizes[receiver] == 0), 0, jnp.maximum(margin, 0))
    moved = jax.random.randint(jax.random.fold_in(own, 4), (number_of // 2,), 0, 1 << 20) % (margin + 1)
    sizes = sizes.at[donor].add(-moved).at[receiver].add(moved)
    items = jnp.searchsorted(jnp.cumsum(sizes), jnp.arange(rows * top), side="right").astype(jnp.int32)
    table = items.reshape(top, rows).T
    table = table[jax.random.permutation(jax.random.fold_in(own, 1), rows)]
    turn = jax.random.randint(jax.random.fold_in(own, 2), (rows, 1), 0, top)
    return jnp.take_along_axis(table, (jnp.arange(top)[None, :] + turn) % top, axis=1)


def portions_of(number_of, total, bound, lean, full):
    portions = [(1 << 20) // math.isqrt(grade ** lean) + 1 for grade in range(1, number_of + 1)]
    largest = bound if full else min(bound, max(-(-total // number_of), total * portions[0] // sum(portions)))
    least = 1 if total - largest >= number_of - 1 else 0
    given, spare = [largest] + [least] * (number_of - 1), total - largest - least * (number_of - 1)
    while spare > 0:
        free = [i for i in range(1, number_of) if given[i] < largest] or [i for i in range(1, number_of) if given[i] < bound]
        whole, remaining = sum([portions[i] for i in free]), spare
        for i in free:
            extra = min(bound - given[i], max(1, remaining * portions[i] // whole), spare)
            given[i] = given[i] + extra
            spare = spare - extra
    return np.array(given)


def scatter_about(stream_key, shape, scale, reach, cuts=(), held_as=jnp.bfloat16):
    array = jax.random.normal(stream_key, shape, jnp.float32) * scale
    if len(cuts) > 0:
        array = block_scale(stream_key, shape, cuts, -0.22, 0.18) * array
    return jnp.clip(array, min=-reach, max=reach).astype(held_as)


def setup_inputs(seed: int = 0, part: int = 0) -> dict:
    streams_of = jax.random.split(jax.random.key(seed), 19)
    own_keys = jax.random.split(jax.random.fold_in(streams_of[18], part), 19)
    tokens = scatter_about(own_keys[0], (SEQS, D), 1.0, 6.0, ((0, 16),))
    cache_latent = scatter_about(own_keys[1], (SEQS, CACHE, LATENT), 1.0, 6.0, ((0, 16),))
    cache_rope = draw_cache_rope(jax.random.fold_in(jax.random.fold_in(streams_of[18], part), 71), part)
    lengths = draw_lengths(jax.random.fold_in(jax.random.fold_in(streams_of[18], part), 71), part)
    w_query = scatter_about(streams_of[4], (D, HEADS * (NOPE + ROPE)), D ** -0.5, 0.125, ((0, 16),))
    w_latent = scatter_about(streams_of[5], (D, LATENT), D ** -0.5, 0.125, ((0, 16),))
    w_rope = scatter_about(streams_of[6], (D, ROPE), D ** -0.5, 0.125, ((0, 16),))
    w_absorb = scatter_about(streams_of[7], (LATENT, HEADS * NOPE), LATENT ** -0.5, 0.25)
    w_value = scatter_about(streams_of[8], (LATENT, HEADS * VDIM), LATENT ** -0.5, 0.25)
    w_output = scatter_about(streams_of[9], (HEADS * VDIM, D), (HEADS * VDIM) ** -0.5, 0.1875, ((0, 16),))
    gain_attn = jnp.clip(1.0 + 0.18 * jax.random.normal(streams_of[10], (D,), jnp.float32), 0.1, 1.9)
    gain_latent = jnp.clip(1.0 + 0.18 * jax.random.normal(streams_of[11], (LATENT,), jnp.float32), 0.1, 1.9)
    gain_moe = jnp.clip(1.0 + 0.18 * jax.random.normal(streams_of[12], (D,), jnp.float32), 0.1, 1.9)
    routes_keys = jax.random.split(jax.random.fold_in(own_keys[13], 1), SEQS // SEQS)
    routes_turns = jax.random.permutation(jax.random.fold_in(own_keys[13], 3), SEQS // SEQS)
    routes = jax.vmap(lambda own, number: assign_block(jax.random.fold_in(own_keys[13], 2), own, number, SEQS, EXPERTS, TOPK, CAP, 2))(routes_keys, routes_turns).reshape((SEQS, TOPK))
    route_scores = jnp.clip(jnp.exp(math.log(1.0) - 1.609438 * jax.random.uniform(own_keys[14], (SEQS, TOPK), jnp.float32) ** block_scale(own_keys[14], (SEQS, TOPK), ((0, 16),), -0.2, 0.2)), 0.2, 1.0)
    w_gate = scatter_about(streams_of[15], (EXPERTS, D, FF), D ** -0.5, 0.125, ((0, 16),))
    w_up = scatter_about(streams_of[16], (EXPERTS, D, FF), D ** -0.5, 0.125, ((0, 16),))
    w_down = scatter_about(streams_of[17], (EXPERTS, FF, D), FF ** -0.5, 0.25, ((0, 16),))
    return {"tokens": tokens, "cache_latent": cache_latent, "cache_rope": cache_rope, "lengths": lengths, "w_query": w_query, "w_latent": w_latent, "w_rope": w_rope, "w_absorb": w_absorb, "w_value": w_value, "w_output": w_output, "gain_attn": gain_attn, "gain_latent": gain_latent, "gain_moe": gain_moe, "routes": routes, "route_scores": route_scores, "w_gate": w_gate, "w_up": w_up, "w_down": w_down}


EPS = 1e-06
THETA = 10000.0

def rms_scale(values, gain):
    return values * lax.rsqrt(lax.optimization_barrier(jnp.mean(values * values, axis=-1, keepdims=True)) + EPS) * gain.astype(jnp.float32)

def rope_tables(positions, width):
    inverse = THETA ** (-jnp.arange(0, width, 2).astype(jnp.float32) / width)
    angle = positions.astype(jnp.float32)[:, None] * inverse[None, :]
    return (jnp.cos(angle), jnp.sin(angle))

def apply_rope(values, cosine, sine):
    half = values.shape[-1] // 2
    first, second = (values[..., :half], values[..., half:])
    return jnp.concatenate([first * cosine - second * sine, second * cosine + first * sine], axis=-1)

def attend_one(items):
    q_abs, q_pe, lat_cache, rope_cache, ckv, kpe, length = items
    scale = (NOPE + ROPE) ** (-0.5)
    past = (jnp.einsum('hc,kc->hk', q_abs.astype(jnp.float32), lat_cache.astype(jnp.float32)) + jnp.einsum('hr,rk->hk', q_pe.astype(jnp.float32), rope_cache.astype(jnp.float32))) * scale
    fresh = (jnp.einsum('hc,c->h', q_abs.astype(jnp.float32), ckv.astype(jnp.float32)) + jnp.einsum('hr,r->h', q_pe.astype(jnp.float32), kpe.astype(jnp.float32))) * scale
    valid = jnp.arange(lat_cache.shape[0]).astype(jnp.int32)[None, :] < length
    top = jnp.maximum(lax.optimization_barrier(jnp.max(jnp.where(valid, past, -jnp.inf), axis=-1)), fresh)
    e_past = jnp.where(valid, jnp.exp(past - top[:, None]), 0.0)
    e_new = jnp.exp(fresh - top)
    total = lax.optimization_barrier(jnp.sum(e_past, axis=-1)) + e_new
    p_past = (e_past / total[:, None]).astype(jnp.bfloat16)
    p_new = (e_new / total).astype(jnp.bfloat16)
    out = jnp.einsum('hk,kc->hc', p_past.astype(jnp.float32), lat_cache.astype(jnp.float32)) + p_new.astype(jnp.float32)[:, None] * ckv.astype(jnp.float32)[None, :]
    return out.astype(jnp.bfloat16)

def reference(tokens, cache_latent, cache_rope, lengths, w_query, w_latent, w_rope, w_absorb, w_value, w_output, gain_attn, gain_latent, gain_moe, routes, route_scores, w_gate, w_up, w_down):
    count = tokens.shape[0]
    normed = rms_scale(tokens.astype(jnp.float32), gain_attn).astype(jnp.bfloat16)
    query = jnp.dot(normed, w_query, preferred_element_type=jnp.float32).astype(jnp.bfloat16)
    latent_raw = jnp.dot(normed, w_latent, preferred_element_type=jnp.float32).astype(jnp.bfloat16)
    rope_raw = jnp.dot(normed, w_rope, preferred_element_type=jnp.float32).astype(jnp.bfloat16)
    new_latent = rms_scale(latent_raw.astype(jnp.float32), gain_latent).astype(jnp.bfloat16)
    cosine, sine = rope_tables(lengths, ROPE)
    new_rope = apply_rope(rope_raw.astype(jnp.float32), cosine, sine).astype(jnp.bfloat16)
    heads_view = query.reshape(count, HEADS, NOPE + ROPE)
    q_nope = heads_view[:, :, :NOPE]
    q_pe = apply_rope(heads_view[:, :, NOPE:].astype(jnp.float32), cosine[:, None, :], sine[:, None, :]).astype(jnp.bfloat16)
    q_abs = jnp.einsum('shn,chn->shc', q_nope.astype(jnp.float32), w_absorb.reshape(LATENT, HEADS, NOPE).astype(jnp.float32)).astype(jnp.bfloat16)
    attended = lax.map(attend_one, (q_abs, q_pe, cache_latent, cache_rope, new_latent, new_rope, lengths))
    values = jnp.einsum('shc,chv->shv', attended.astype(jnp.float32), w_value.reshape(LATENT, HEADS, VDIM).astype(jnp.float32)).astype(jnp.bfloat16)
    attn_out = jnp.dot(values.reshape(count, HEADS * VDIM), w_output, preferred_element_type=jnp.float32)
    resid = (tokens.astype(jnp.float32) + attn_out).astype(jnp.bfloat16)
    moe_in = rms_scale(resid.astype(jnp.float32), gain_moe).astype(jnp.bfloat16)

    def expert_one(items):
        index, row = items
        gate = jnp.dot(row[None, :], w_gate[index], preferred_element_type=jnp.float32)
        upper = jnp.dot(row[None, :], w_up[index], preferred_element_type=jnp.float32)
        hidden = (jax.nn.silu(gate) * upper).astype(jnp.bfloat16)
        return jnp.dot(hidden, w_down[index], preferred_element_type=jnp.float32).astype(jnp.bfloat16)[0]
    flat_ids = routes.reshape(-1).astype(jnp.int32)
    flat_rows = jnp.repeat(moe_in, TOPK, axis=0)
    expert_out = lax.map(expert_one, (flat_ids, flat_rows)).reshape(count, TOPK, D)
    route_weight = route_scores / lax.optimization_barrier(jnp.sum(route_scores, axis=-1, keepdims=True))
    moe_sum = lax.optimization_barrier(jnp.sum(route_weight[:, :, None] * expert_out.astype(jnp.float32), axis=1))
    mixed = (resid.astype(jnp.float32) + moe_sum).astype(jnp.bfloat16)
    return (mixed, new_latent, new_rope)
```

```python
import functools
import math
import jax
import jax.numpy as jnp
from jax import lax
from jax.experimental import pallas as pl
from jax.experimental.pallas import tpu as pltpu
from jax.sharding import PartitionSpec as P

HEADS = 16
NOPE = 64
ROPE = 32
VDIM = 64
EPS = 1e-06
THETA = 10000.0
LANES = 128
CHUNKS = 2
EXACT = 8
FIRST = 3
F32 = jnp.float32
BF16 = jnp.bfloat16
MESH = pl.DeviceIdType.MESH


def dot(a, b):
    return jnp.dot(a, b, preferred_element_type=F32)


def dot_t(a, b):
    return lax.dot_general(a, b, (((1,), (1,)), ((), ())), preferred_element_type=F32)


def iota(shape, dim):
    return lax.broadcasted_iota(jnp.int32, shape, dim)


def ones_where(mask):
    return jnp.where(mask, 1.0, 0.0).astype(BF16)


def rms_dense(values, gain, size):
    total = jnp.sum(jnp.sum(values * values, axis=1, keepdims=True), axis=0, keepdims=True)
    return values * lax.rsqrt(total * (1.0 / size) + EPS) * gain


def rope_tables(position):
    half = ROPE // 2
    lane = iota((1, LANES), 1) & (ROPE - 1)
    step = lane & (half - 1)
    inverse = jnp.zeros((1, LANES), F32)
    for i in range(half):
        inverse = jnp.where(step == i, THETA ** (-2.0 * i / ROPE), inverse)
    angle = position.astype(F32) * inverse
    sine = jnp.sin(angle)
    return jnp.cos(angle), jnp.where(lane < half, -sine, sine)


def rotate(values, cosine, sine):
    half = ROPE // 2
    low = (iota(values.shape, 1) & (ROPE - 1)) < half
    swapped = jnp.where(low, pltpu.roll(values, LANES - half, 1), pltpu.roll(values, half, 1))
    return values * cosine + swapped * sine


def split_heads(heads):
    group = heads * (NOPE + ROPE)
    src, col = iota((group, group), 0), iota((group, group), 1)
    first = (NOPE + ROPE) * (col // NOPE) + (col & (NOPE - 1))
    rest = col - heads * NOPE
    second = (NOPE + ROPE) * (rest // ROPE) + NOPE + (rest & (ROPE - 1))
    return ones_where(src == jnp.where(col < heads * NOPE, first, second))


def rows_to_lanes(values, first, count, heads):
    return [jnp.broadcast_to(values[first + r : first + r + 1, :], (heads, LANES)) for r in range(count)]


def kernel(
    n, hubs,
    tok_hbm, g_attn_hbm, g_lat_hbm, g_moe_hbm, len_hbm, route_hbm, score_hbm,
    cache_hbm, crope_hbm, wq_hbm, wl_hbm, wr_hbm, wa_hbm, wv_hbm, wo_hbm, wg_hbm, wu_hbm, wd_hbm,
    mixed_ref, nlat_ref, nrope_ref,
    tok, g_attn, g_lat, g_moe, length, route, score,
    cache, wq, wl, wr, wa, wv, wo, wg, wu, wd, wqn, wocol, cache_t, wa_t, dense,
    send1, recv1, stage, send2, recv2, send2r, recv2r, stage3, send3, recv3, send4, recv4,
    send6, recv6, local_sem, link_sem, hub_sem,
):
    me = lax.axis_index("ep")
    barrier = pltpu.get_barrier_semaphore()
    upper = me // (n // 2)

    def far_first(k):
        return upper * k + (1 - upper) * (n - 1 - k)

    def each_peer(act):
        own = far_first(me)

        def step(k, carry):
            act(far_first(k))
            return carry

        lax.fori_loop(0, own, step, 0)
        lax.fori_loop(own + 1, n, step, 0)

    each_peer(
        lambda peer: pl.semaphore_signal(barrier, inc=1, device_id={"ep": peer}, device_id_type=MESH)
    )
    depth, width = wq_hbm.shape[0], wo_hbm.shape[0]
    share = LANES // depth
    cut = width * FIRST // 32 * 8
    mine = pl.ds(pl.multiple_of(depth * lax.rem(me, share), depth), depth)
    block = me // share
    tall = tok.shape[1] // LANES
    cols = tok.shape[1] // hubs
    per_hub = cols // LANES
    base = (n - 2 * hubs) // 2

    def hub_device(h):
        return base + 2 * h + 1

    def near_first(i):
        return upper * (hubs - 1 - i) + (1 - upper) * i

    my_hub = (me - base) // 2
    is_hub = (lax.rem(me, 2) == 1) & (me >= base) & (me < base + 2 * hubs)

    def columns(h):
        return pl.ds(pl.multiple_of(h * cols, cols), cols)

    def band(owner, size):
        return pl.ds(pl.multiple_of(owner * size, size), size)

    if share > 1:
        for w in (wq, wl, wr):
            w[...] = jnp.zeros_like(w)
    pairs = [
        (tok_hbm, tok), (g_attn_hbm, g_attn), (len_hbm, length), (wq_hbm, wq.at[mine]),
        (wl_hbm, wl.at[mine]), (wr_hbm, wr if share == 1 else wr.at[mine]), (wo_hbm, wo),
        (g_lat_hbm, g_lat), (g_moe_hbm, g_moe), (route_hbm, route), (score_hbm, score),
        (cache_hbm.at[0], cache), (wa_hbm, wa), (crope_hbm.at[0], cache_t.at[wl_hbm.shape[1] :]), (wv_hbm, wv),
        (wg_hbm.at[0], wg), (wu_hbm.at[0], wu), (wd_hbm.at[0], wd),
    ]
    loads = [pltpu.make_async_copy(a, b, local_sem.at[i]) for i, (a, b) in enumerate(pairs)]
    for load in loads:
        load.start()
    (
        l_tok, l_ga, l_len, l_wq, l_wl, l_wr, l_wo, l_gl, l_gm, l_route, l_score, l_cache, l_wa,
        l_crope, l_wv, l_wg, l_wu, l_wd,
    ) = loads

    def launch(peer, source, target, sent, received):
        pltpu.make_async_remote_copy(
            src_ref=source,
            dst_ref=target,
            send_sem=sent,
            recv_sem=received,
            device_id={"ep": peer},
            device_id_type=MESH,
        ).start()

    def send(phase, source, target):
        each_peer(
            lambda peer: launch(
                peer, source(peer), target, link_sem.at[0, phase], link_sem.at[1, phase]
            )
        )

    def await_bytes(ref, sem):
        pltpu.make_async_copy(ref, ref, sem).wait()

    def drain(side, phase, target):
        await_bytes(target.at[pl.ds(0, (n - 1) * (target.shape[0] // n))], link_sem.at[side, phase])

    def each_hub(act):
        for i in range(hubs):
            h = near_first(hubs - 1 - i)

            @pl.when(me != hub_device(h))
            def _():
                act(h)

    def reshard(half):
        low, high = (cut, width) if half else (0, cut)
        rows = pl.ds(pl.multiple_of(me * width + low, 8), high - low)
        source = lambda h: wo.at[low:high, columns(h)]
        each_hub(
            lambda h: launch(
                hub_device(h), source(h), wocol.at[rows], link_sem.at[0, 4 + half],
                link_sem.at[1, 4 + half],
            )
        )

        @pl.when(is_hub)
        def _():
            wocol[rows, :] = wo[low:high, columns(my_hub)]

    l_tok.wait()
    l_ga.wait()
    tokens = tok[...].astype(F32)
    for r in range(tall):
        dense[r : r + 1, :] = tokens[:, r * LANES : (r + 1) * LANES]
    tokens = dense[...]
    normed = rms_dense(tokens, g_attn[...], tok.shape[1]).astype(BF16).astype(F32)
    for r in range(tall):
        send1[r] = normed[r : r + 1, :]
    pl.semaphore_wait(barrier, n - 1)
    send(0, lambda peer: send1.at[peer // share], recv1.at[me])
    recv1[me] = send1[block]
    l_wo.wait()
    reshard(0)

    qw, lw = wq.shape[1], wl.shape[1]
    tiles = wv.shape[1] // LANES
    slot = send3.shape[1]
    for h in range(hubs):
        stage3[h * slot + tiles : h * slot + tiles + per_hub, :] = tokens[
            h * per_hub : (h + 1) * per_hub, :
        ]
    l_wq.wait()
    few = LANES // ROPE
    order = split_heads(few)
    span = few * (NOPE + ROPE)
    nope_rows, pe_rows, lat_rows = HEADS * NOPE // LANES, HEADS * ROPE // LANES, lw // LANES
    for g in range(HEADS // few):
        moved = dot(wq[:, g * span : (g + 1) * span], order).astype(BF16)
        wqn[:, g * few * NOPE : (g + 1) * few * NOPE] = moved[:, : few * NOPE]
        start = HEADS * NOPE + g * LANES
        wqn[:, start : start + LANES] = moved[:, few * NOPE :]
    l_len.wait()
    cosine, sine = rope_tables(jnp.full((1, LANES), length[0]))
    l_wl.wait()
    l_wr.wait()
    edge = 2 * LANES
    same = ones_where(iota((edge, edge), 0) == iota((edge, edge), 1))

    def turn(source, target):
        for i in range(source.shape[0] // edge):
            for j in range(source.shape[1] // edge):
                part = source[i * edge : (i + 1) * edge, j * edge : (j + 1) * edge]
                target[j * edge : (j + 1) * edge, i * edge : (i + 1) * edge] = dot_t(same, part).astype(BF16)

    l_cache.wait()
    turn(cache, cache_t)
    drain(1, 0, recv1)
    rows = jnp.concatenate([recv1[t] for t in range(n)], axis=0).astype(BF16)
    wide = (qw + lw) // LANES
    part_q = dot(rows, wqn[...])
    for j in range(qw // LANES):
        stage[pl.ds(j, n, stride=wide), :] = part_q[:, j * LANES : (j + 1) * LANES]
    part_l = dot(rows, wl[...])
    for j in range(lat_rows):
        stage[pl.ds(qw // LANES + j, n, stride=wide), :] = part_l[:, j * LANES : (j + 1) * LANES]
    part_r = dot_t(rows, wr[...]) if share == 1 else dot(rows, wr[...])
    for j in range(pe_rows):
        at = (nope_rows + j) * LANES
        send2r[pl.ds(j, n, stride=EXACT), :] = part_q[:, at : at + LANES]
    part_r = jnp.concatenate([part_r, jnp.zeros((n, LANES - ROPE), F32)], axis=1)
    send2r[pl.ds(pe_rows, n, stride=EXACT), :] = part_r
    send2[...] = stage[...].astype(BF16).reshape(send2.shape)

    def send_sums(peer):
        launch(
            peer, send2r.at[band(peer, EXACT)], recv2r.at[band(me, EXACT)], link_sem.at[0, 2],
            link_sem.at[1, 2],
        )
        launch(peer, send2.at[peer], recv2.at[me], link_sem.at[0, 1], link_sem.at[1, 1])

    each_peer(send_sums)
    recv2[me] = send2[me]
    recv2r[band(me, EXACT), :] = send2r[band(me, EXACT), :]
    drain(0, 0, recv1)
    l_gl.wait()
    l_wa.wait()
    turn(wa, wa_t)
    l_crope.wait()
    l_wv.wait()
    head = iota((HEADS, LANES), 0)
    lane = iota((HEADS, LANES), 1)
    drain(1, 1, recv2)
    drain(1, 2, recv2r)
    reshard(1)
    summed = recv2[0].astype(F32)
    exact = recv2r[:EXACT, :]
    for t in range(1, n):
        summed = summed + recv2[t].astype(F32)
        exact = exact + recv2r[t * EXACT : (t + 1) * EXACT, :]
    exact = exact.astype(BF16).astype(F32)
    summed = summed.astype(BF16).astype(F32)
    first = nope_rows + pe_rows
    new_latent = rms_dense(summed[first:, :], g_lat[...], lw).astype(BF16).astype(F32)
    rotated = rotate(exact, cosine, sine)
    new_rope = rotated[pe_rows : pe_rows + 1, :].astype(BF16)
    for r in range(lat_rows):
        nlat_ref[:, r * LANES : (r + 1) * LANES] = new_latent[r : r + 1, :].astype(BF16)
    nrope_ref[...] = new_rope[:, :ROPE]
    new_rope = new_rope.astype(F32)
    per = LANES // NOPE
    q_diag = jnp.concatenate(
        [
            jnp.where(head == per * r + lane // NOPE, row, 0.0)
            for r, row in enumerate(rows_to_lanes(summed, 0, nope_rows, HEADS))
        ],
        axis=1,
    ).astype(BF16)
    q_abs = dot(q_diag, wa_t[...]).astype(BF16)
    q_pe = jnp.zeros((HEADS, LANES), F32)
    for r, row in enumerate(rows_to_lanes(rotated, 0, pe_rows, HEADS)):
        q_pe = jnp.where(head == few * r + lane // ROPE, row, q_pe)
    shift = LANES // 2
    while shift >= ROPE:
        q_pe = q_pe + pltpu.roll(q_pe, shift, 1)
        shift //= 2
    q_pe = q_pe[:, :ROPE].astype(BF16)
    unit = (NOPE + ROPE) ** (-0.5) * math.log2(math.e)
    lat_row = jnp.concatenate(rows_to_lanes(new_latent, 0, lat_rows, HEADS), axis=1)
    fresh = jnp.sum(q_abs.astype(F32) * lat_row, axis=-1, keepdims=True) + jnp.sum(
        q_pe.astype(F32) * new_rope[:, :ROPE], axis=-1, keepdims=True
    )
    chunk = cache.shape[0] // CHUNKS
    query = jnp.concatenate([q_abs, q_pe], axis=1)
    pasts = [dot(query, cache_t[:, c * chunk : (c + 1) * chunk]) for c in range(CHUNKS)]
    tops, sums, outs = [], [], []
    for c, past in enumerate(pasts):
        past = jnp.where(iota(past.shape, 1) < length[0] - c * chunk, past, -jnp.inf)
        top = jnp.maximum(jnp.max(past, axis=-1, keepdims=True), fresh)
        e_past = jnp.exp2((past - top) * unit)
        tops.append(top)
        sums.append(jnp.sum(e_past, axis=-1, keepdims=True))
        outs.append(dot(e_past.astype(BF16), cache[c * chunk : (c + 1) * chunk, :]))
    top = functools.reduce(jnp.maximum, tops)
    e_new = jnp.exp2((fresh - top) * unit)
    total, mixed = e_new, e_new * lat_row
    for peak, part, out in zip(tops, sums, outs):
        weight = jnp.exp2((peak - top) * unit)
        total = total + part * weight
        mixed = mixed + out * weight
    attended = (mixed / total).astype(BF16)
    values = dot(attended, wv[...])
    for j in range(tiles):
        part = values[:, j * LANES : (j + 1) * LANES]
        part = jnp.where(head == (LANES // VDIM) * j + lane // VDIM, part, 0.0)
        part = jnp.sum(part, axis=0, keepdims=True)
        for h in range(hubs):
            stage3[h * slot + j : h * slot + j + 1, :] = part
    send3[...] = stage3[...].astype(BF16).reshape(send3.shape)
    each_hub(
        lambda h: launch(
            hub_device(h), send3.at[h], recv3.at[me], link_sem.at[0, 3], link_sem.at[1, 3]
        )
    )
    drain(0, 1, send2)
    drain(0, 2, send2r)

    @pl.when(is_hub)
    def _():
        recv3[me] = send3[my_hub]
        drain(1, 4, wocol.at[pl.ds(0, n * cut)])
        drain(1, 5, wocol.at[pl.ds(0, n * (width - cut))])
        drain(1, 3, recv3)
        flat = stage.at[pl.ds(0, n * slot)]
        flat[...] = recv3[...].astype(F32).reshape(flat.shape)
        rows = [flat[pl.ds(j, n, stride=slot), :].astype(BF16) for j in range(tiles)]
        raw = [flat[pl.ds(tiles + j, n, stride=slot), :] for j in range(per_hub)]
        part = dot(jnp.concatenate(rows, axis=1), wocol[...])
        send4[...] = (jnp.concatenate(raw, axis=1) + part).astype(BF16)

        def spread(k, carry):
            j = lax.rem(2 * k, n) + (2 * k) // n
            peer = upper * j + (1 - upper) * (n - 2 - 2 * (j // 2) + lax.rem(j, 2))

            @pl.when(peer != me)
            def _():
                launch(peer, send4, recv4.at[my_hub], link_sem.at[0, 6], hub_sem.at[my_hub])

            return carry

        lax.fori_loop(0, n, spread, 0)
        recv4[my_hub] = send4[...]

    l_gm.wait()
    l_wg.wait()
    l_wu.wait()
    l_wd.wait()
    half = wg.shape[1] // 2
    parts = [slice(0, half), slice(half, 2 * half)]
    gates = [jnp.zeros((n, half), F32) for _ in parts]
    lifts = [jnp.zeros((n, half), F32) for _ in parts]
    power = jnp.zeros((n, LANES), F32)
    for i in range(hubs):
        h = near_first(i)

        @pl.when(me != hub_device(h))
        def _():
            await_bytes(recv4.at[h], hub_sem.at[h])

        part = recv4[h].astype(F32)
        for j in range(per_hub):
            piece = part[:, j * LANES : (j + 1) * LANES]
            power = power + piece * piece
        gains = [
            part[:, j * LANES : (j + 1) * LANES] * g_moe[pl.ds(h * per_hub + j, 1), :]
            for j in range(per_hub)
        ]
        rows = jnp.concatenate(gains, axis=1).astype(BF16)
        for q, at in enumerate(parts):
            gates[q] = gates[q] + dot(rows, wg[columns(h), at])
            lifts[q] = lifts[q] + dot(rows, wu[columns(h), at])
    scale = lax.rsqrt(jnp.sum(power, axis=1, keepdims=True) * (1.0 / tok.shape[1]) + EPS)
    hidden = [
        (jax.nn.silu(gate * scale) * (lift * scale)).astype(BF16)
        for gate, lift in zip(gates, lifts)
    ]
    result = dot(hidden[0], wd[parts[0], :]) + dot(hidden[1], wd[parts[1], :])
    for j in range(tall):
        stage[pl.ds(j, n, stride=tall), :] = result[:, j * LANES : (j + 1) * LANES]
    send6[...] = stage[pl.ds(0, n * tall), :].astype(BF16).reshape(send6.shape)
    send(7, lambda peer: send6.at[peer], recv6.at[me])
    recv6[me] = send6[me]
    for h in range(hubs):
        part = recv4[h].astype(F32)
        for j in range(per_hub):
            stage[pl.ds(h * per_hub + j, n, stride=tall), :] = part[:, j * LANES : (j + 1) * LANES]
    resid = stage[band(me, tall), :]
    each_hub(lambda h: await_bytes(send3.at[h], link_sem.at[0, 3]))
    for half, size in enumerate((cut, width - cut)):
        each_hub(
            lambda h: await_bytes(wocol.at[pl.ds(0, size)], link_sem.at[0, 4 + half])
        )

    @pl.when(is_hub)
    def _():
        def step(k, carry):
            await_bytes(send4, link_sem.at[0, 6])
            return carry

        lax.fori_loop(1, n, step, 0)

    l_route.wait()
    l_score.wait()
    topk = route.shape[1]
    weight = score[0, 0]
    for k in range(1, topk):
        weight = weight + score[0, k]
    shares = [jnp.full(resid.shape, score[0, k]) / weight for k in range(topk)]
    drain(1, 7, recv6)
    moe_sum = shares[0] * recv6[route[0, 0]].astype(F32)
    for k in range(1, topk):
        moe_sum = moe_sum + shares[k] * recv6[route[0, k]].astype(F32)
    mixed = resid + moe_sum
    for r in range(tall):
        mixed_ref[:, r * LANES : (r + 1) * LANES] = mixed[r : r + 1, :].astype(BF16)
    drain(0, 7, send6)


def finish(mixed, nlat, nrope, mixed_hbm, nlat_hbm, nrope_hbm, sem):
    pairs = [(mixed, mixed_hbm), (nlat, nlat_hbm), (nrope, nrope_hbm)]
    copies = [pltpu.make_async_copy(a, b, sem.at[i]) for i, (a, b) in enumerate(pairs)]
    for copy in copies:
        copy.start()
    for copy in copies:
        copy.wait()


def body(
    tokens, cache_latent, cache_rope, lengths, w_query, w_latent, w_rope, w_absorb, w_value,
    w_output, gain_attn, gain_latent, gain_moe, routes, route_scores, w_gate, w_up, w_down,
):
    n = lax.axis_size("ep")
    d = tokens.shape[1]
    qw, lw = w_query.shape[1], w_latent.shape[1]
    tall, wide = d // LANES, (qw + lw) // LANES
    vmem = pl.BlockSpec(memory_space=pltpu.VMEM)
    hbm = pl.BlockSpec(memory_space=pltpu.HBM)
    lat, gain, moe = (g.reshape(-1, LANES) for g in (gain_latent, gain_attn, gain_moe))

    def like(a):
        return pltpu.VMEM(a.shape[-2:], a.dtype)

    depth = w_query.shape[0]
    turned = depth == LANES
    if turned:
        w_rope = w_rope.T
    hubs = min(n // 4, tall)
    row = lambda count, size: pltpu.VMEM((count, 1, size), F32)
    tile = lambda count, size: pltpu.VMEM((count, size, LANES), BF16)
    outs = (
        jax.ShapeDtypeStruct(tokens.shape, BF16),
        jax.ShapeDtypeStruct((1, lw), BF16),
        jax.ShapeDtypeStruct((1, ROPE), BF16),
    )
    made = pl.pallas_call(
        functools.partial(kernel, n, hubs),
        out_shape=tuple(pltpu.VMEM(o.shape, o.dtype) for o in outs),
        in_specs=[hbm] * 18,
        out_specs=(vmem, vmem, vmem),
        scratch_shapes=[
            like(tokens), like(gain), like(lat), like(moe),
            pltpu.SMEM(lengths.shape, lengths.dtype), pltpu.SMEM(routes.shape, routes.dtype),
            pltpu.SMEM(route_scores.shape, route_scores.dtype),
            like(cache_latent), pltpu.VMEM((LANES, qw), BF16),
            pltpu.VMEM((LANES, lw), BF16), pltpu.VMEM((ROPE, LANES) if turned else (LANES, ROPE), BF16),
            like(w_absorb), like(w_value), like(w_output), like(w_gate), like(w_up), like(w_down),
            pltpu.VMEM((LANES, qw), BF16), pltpu.VMEM((n * w_output.shape[0], d // hubs), BF16),
            pltpu.VMEM((lw + ROPE, cache_latent.shape[1]), BF16), pltpu.VMEM(w_absorb.shape[::-1], BF16),
            pltpu.VMEM((tall, LANES), F32),
            row(tall, LANES), row(n, LANES), pltpu.VMEM((n * max(tall, wide), LANES), F32),
            tile(n, wide), tile(n, wide), pltpu.VMEM((n * EXACT, LANES), F32),
            pltpu.VMEM((n * EXACT, LANES), F32),
            pltpu.VMEM((hubs * 16, LANES), F32), tile(hubs, 16), tile(n, 16),
            pltpu.VMEM((n, d // hubs), BF16), pltpu.VMEM((hubs, n, d // hubs), BF16),
            tile(n, tall), tile(n, tall),
            pltpu.SemaphoreType.DMA((18,)),
            pltpu.SemaphoreType.DMA((2, 8)),
            pltpu.SemaphoreType.DMA((hubs,)),
        ],
        compiler_params=pltpu.CompilerParams(
            collective_id=0, has_side_effects=True, vmem_limit_bytes=56 * 1024 * 1024
        ),
    )(
        tokens, gain, lat, moe, lengths, routes, route_scores, cache_latent, cache_rope, w_query,
        w_latent, w_rope, w_absorb, w_value, w_output, w_gate, w_up, w_down,
    )
    return pl.pallas_call(
        finish,
        out_shape=outs,
        in_specs=[vmem] * 3,
        out_specs=[hbm] * 3,
        scratch_shapes=[pltpu.SemaphoreType.DMA((3,))],
    )(*[pltpu.with_memory_space_constraint(m, pltpu.VMEM) for m in made])


def solution(mesh):
    rows = P(("grp", "ep"), None)
    cube = P(("grp", "ep"), None, None)
    split = P("ep", None)
    placed = (
        rows, cube, cube, P(("grp", "ep")), split, split, split, P(), P(), split, P(), P(), P(),
        rows, rows, P("ep", None, None), P("ep", None, None), P("ep", None, None),
    )
    return jax.shard_map(
        body, mesh=mesh, in_specs=placed, out_specs=(rows, rows, rows), check_vma=False
    )
```
